32 devices in a mesh: kv: 8 (over z, x), tp: 4 (over y, core).
Axes of the slice: x: 2, y: 2, z: 4, core: 2. Of those that a mesh axis runs over, the one named last changes fastest.
Arguments:
- tokens: bfloat16 [256, 2048], P('kv', 'tp'), may hold values from -60 to 60, as said below
- memory: float32 [256, 8, 128, 128], P('kv', 'tp'), may hold values from -0.6 to 0.6
- normalizer: float32 [256, 8, 128], P('kv', 'tp'), may hold values from -0.6 to 0.6
- stabilizer: float32 [256, 8], P('kv', 'tp'), may hold values from -4 to 4
- norm_gain: float32 [2048], replicated, may hold values from 0.1 to 1.9
- query_weight: bfloat16 [2048, 1024], P(None, 'tp'), may hold values from -0.125 to 0.125
- key_weight: bfloat16 [2048, 1024], P(None, 'tp'), may hold values from -0.125 to 0.125
- value_weight: bfloat16 [2048, 1024], P(None, 'tp'), may hold values from -0.125 to 0.125
- outgate_weight: bfloat16 [2048, 1024], P(None, 'tp'), may hold values from -0.125 to 0.125
- input_gate_weight: bfloat16 [2048, 8], replicated, may hold values from -0.125 to 0.125
- forget_gate_weight: bfloat16 [2048, 8], replicated, may hold values from -0.125 to 0.125
- forget_bias: float32 [8], replicated, may hold values from -1 to 5
- memory_gain: float32 [1024], P('tp'), may hold values from 0.1 to 1.9
- proj_weight: bfloat16 [1024, 2048], P(None, 'tp'), may hold values from -0.1875 to 0.1875
- ffn_gain: float32 [2048], P('tp'), may hold values from 0.1 to 1.9
- up_weight: bfloat16 [2048, 8192], P('tp', 'kv'), may hold values from -0.125 to 0.125
- down_weight: bfloat16 [8192, 2048], P('kv', 'tp'), may hold values from -0.0625 to 0.0625
Outputs:
- layer_out: bfloat16 [256, 2048], P('kv', 'tp')
- memory_new: float32 [256, 8, 128, 128], P('kv', 'tp')
- normalizer_new: float32 [256, 8, 128], P('kv', 'tp')
- stabilizer_new: float32 [256, 8], P('kv', 'tp')
The draws below stay inside these ranges and needn't reach their ends.
Inputs may be any that keep to these rules, and one draw needn't show every extreme that they name: `tokens`: activations whose feature blocks and rows differ in scale.
All inputs are finite; a program needn't handle non-finite values.
Results may differ from the reference program's by a relative error of at most 0.0095.
Values may be sent and summed in bfloat16 or wider, within the bound.
A program may use at most 64 MiB of HBM per device.

```python
import math
import jax
import jax.numpy as jnp
from jax import lax

D = 2048
H = 8
DK = 128
DV = 128
FF = 8192
SEQS = 256


def draw_tokens(key, part):
    key_base = jax.random.fold_in(key, 11)
    key_cols = jax.random.fold_in(key, 12)
    key_rows = jax.random.fold_in(key, 13)
    column = jnp.arange(D, dtype=jnp.float32) / (D - 1)
    col_scale = jnp.exp(column * math.log(3.0)) / 1.7 * jnp.exp(jax.random.uniform(key_cols, (D,), jnp.float32, math.log(0.6), math.log(1.6)))
    base = jnp.clip(jax.random.normal(key_base, (SEQS, D), jnp.float32), -4.0, 4.0)
    row_scale = jnp.exp(jax.random.uniform(key_rows, (SEQS, 1), jnp.float32, math.log(0.3), math.log(3.0)))
    return (base * row_scale * col_scale[None, :]).astype(jnp.bfloat16)


def shard_levels(own_key, extent, pieces, low, largest):
    factor_of = 1.0
    for position, blocks in pieces:
        steps = jax.random.uniform(jax.random.fold_in(jax.random.fold_in(own_key, 6), position), (blocks,), jnp.float32, low / len(pieces), largest / len(pieces))
        factor_of = factor_of * jnp.repeat(jnp.exp(steps), extent[position] // blocks).reshape((-1,) + (1,) * (len(extent) - 1 - position))
    return factor_of


def scatter_about(key, extent, width, most, shards=(), kind=jnp.bfloat16):
    values = width * jax.random.normal(key, extent, jnp.float32)
    if shards:
        values = values * shard_levels(key, extent, shards, -0.22, 0.18)
    return jnp.clip(values, -most, most).astype(kind)


def setup_inputs(seed: int = 0) -> dict:
    key_list = jax.random.split(jax.random.key(seed), 18)
    return {
        "tokens": draw_tokens(jax.random.fold_in(key_list[17], 71), 0),
        "memory": scatter_about(key_list[1], (SEQS, H, DV, DK), 0.1, 0.6, ((0, 8), (1, 4)), jnp.float32),
        "normalizer": scatter_about(key_list[2], (SEQS, H, DK), 0.1, 0.6, ((0, 8), (1, 4)), jnp.float32),
        "stabilizer": scatter_about(key_list[3], (SEQS, H), 1.0, 4.0, ((0, 8), (1, 4)), jnp.float32),
        "norm_gain": jnp.clip(1.0 + 0.18 * jax.random.normal(key_list[4], (D,), jnp.float32), 0.1, 1.9),
        "query_weight": scatter_about(key_list[5], (D, H * DK), D ** -0.5, 0.125, ((1, 4),)),
        "key_weight": scatter_about(key_list[6], (D, H * DK), D ** -0.5, 0.125, ((1, 4),)),
        "value_weight": scatter_about(key_list[7], (D, H * DV), D ** -0.5, 0.125, ((1, 4),)),
        "outgate_weight": scatter_about(key_list[8], (D, H * DV), D ** -0.5, 0.125, ((1, 4),)),
        "input_gate_weight": scatter_about(key_list[9], (D, H), D ** -0.5, 0.125),
        "forget_gate_weight": scatter_about(key_list[10], (D, H), D ** -0.5, 0.125),
        "forget_bias": jnp.clip(jax.random.uniform(key_list[11], (H,), jnp.float32, -1.0, 5.0), -1.0, 5.0),
        "memory_gain": jnp.clip(1.0 + 0.18 * jax.random.normal(key_list[12], (H * DV,), jnp.float32), 0.1, 1.9),
        "proj_weight": scatter_about(key_list[13], (H * DV, D), (H * DV) ** -0.5, 0.1875, ((1, 4),)),
        "ffn_gain": jnp.clip(1.0 + 0.18 * jax.random.normal(key_list[14], (D,), jnp.float32), 0.1, 1.9),
        "up_weight": scatter_about(key_list[15], (D, FF), D ** -0.5, 0.125, ((0, 4), (1, 8))),
        "down_weight": scatter_about(key_list[16], (FF, D), FF ** -0.5, 0.0625, ((0, 8), (1, 4))),
    }


EPS = 1e-06

def reference(tokens, memory, normalizer, stabilizer, norm_gain, query_weight, key_weight, value_weight, outgate_weight, input_gate_weight, forget_gate_weight, forget_bias, memory_gain, proj_weight, ffn_gain, up_weight, down_weight):
    rows_f = tokens.astype(jnp.float32)
    scale_one = lax.rsqrt(lax.optimization_barrier(jnp.mean(rows_f * rows_f, axis=-1, keepdims=True)) + EPS)
    normed = (rows_f * scale_one * norm_gain).astype(jnp.bfloat16)
    count = tokens.shape[0]
    query = jnp.dot(normed, query_weight, preferred_element_type=jnp.float32).astype(jnp.bfloat16)
    keys = jnp.dot(normed, key_weight, preferred_element_type=jnp.float32).astype(jnp.bfloat16)
    values = jnp.dot(normed, value_weight, preferred_element_type=jnp.float32).astype(jnp.bfloat16)
    gate_out = jnp.dot(normed, outgate_weight, preferred_element_type=jnp.float32).astype(jnp.bfloat16)
    input_log = jnp.dot(normed, input_gate_weight, preferred_element_type=jnp.float32)
    forget_log = jax.nn.log_sigmoid(jnp.dot(normed, forget_gate_weight, preferred_element_type=jnp.float32) + forget_bias)
    query_f = query.astype(jnp.float32).reshape(count, H, DK)
    keys_f = keys.astype(jnp.float32).reshape(count, H, DK) * DK ** (-0.5)
    values_f = values.astype(jnp.float32).reshape(count, H, DV)
    stab_new = jnp.maximum(forget_log + stabilizer, input_log)
    keep = jnp.exp(forget_log + stabilizer - stab_new)
    admit = jnp.exp(input_log - stab_new)
    memory_new = keep[..., None, None] * memory + admit[..., None, None] * values_f[..., :, None] * keys_f[..., None, :]
    normalizer_new = keep[..., None] * normalizer + admit[..., None] * keys_f
    numer = jnp.einsum('bhed,bhd->bhe', memory_new, query_f, precision=lax.Precision.HIGHEST)
    denom = lax.optimization_barrier(jnp.sum(normalizer_new * query_f, axis=-1))
    cell = numer / jnp.maximum(jnp.abs(denom), 1.0)[..., None]
    mixed = (cell.reshape(count, H * DV) * memory_gain * jax.nn.sigmoid(gate_out.astype(jnp.float32))).astype(jnp.bfloat16)
    second = (rows_f + jnp.dot(mixed, proj_weight, preferred_element_type=jnp.float32)).astype(jnp.bfloat16)
    second_f = second.astype(jnp.float32)
    scale_two = lax.rsqrt(lax.optimization_barrier(jnp.mean(second_f * second_f, axis=-1, keepdims=True)) + EPS)
    scaled = (second_f * ffn_gain).astype(jnp.bfloat16)
    preact = jnp.dot(scaled, up_weight, preferred_element_type=jnp.float32)
    hidden = jnp.square(jax.nn.relu(preact * scale_two)).astype(jnp.bfloat16)
    layer_out = (second_f + jnp.dot(hidden, down_weight, preferred_element_type=jnp.float32)).astype(jnp.bfloat16)
    return (layer_out, memory_new, normalizer_new, stab_new)
```

```python
import functools

import jax
import jax.numpy as jnp
from jax import lax
from jax.experimental import pallas as pl
from jax.experimental.pallas import tpu as pltpu
from jax.sharding import PartitionSpec as P

EPS = 1e-06
LANES = 128
GROUP = 16
LAG2, LAG3, LAG4 = 1, 2, 3
F32, BF16 = jnp.float32, jnp.bfloat16


def dot(a, b):
    return jnp.dot(a, b, preferred_element_type=F32)


def layer_kernel(
    nkv,
    ntp,
    tok,
    mem_h,
    nrm,
    stab,
    ngain,
    wq_h,
    wk_h,
    wv_h,
    wo_h,
    wig,
    wfg,
    fbias,
    mgain,
    wp_h,
    fgain,
    wu_h,
    wd_h,
    out,
    nrm_new,
    stab_new,
    keep_out,
    av_out,
    key_out,
    mem,
    wqkv,
    wp,
    wu,
    wd,
    tokg,
    mixg,
    secg,
    pown,
    xa_s,
    xa_r,
    yb_s,
    yb_r,
    hid,
    hid_r,
    sq_s,
    sq_r,
    part_s,
    part_r,
    down_own,
    w_sem,
    p_sem,
    f_sem,
    m_sem,
    tp_send,
    tp_recv,
    mx_send,
    mx_recv,
    kv_send,
    kv_recv,
    a_send,
    a_recv,
    b_send,
    b_recv,
    c_send,
    c_recv,
    q_send,
    q_recv,
    r_send,
    r_recv,
):
    rows, width = tok.shape
    heads, dk = nrm.shape[1], nrm.shape[2]
    cols = heads * dk
    features = width * ntp
    half = wu.shape[2]
    ny, nz = ntp // 2, nkv // 2
    me_tp, me_kv = lax.axis_index("tp"), lax.axis_index("kv")
    y, core = me_tp // 2, me_tp % 2
    z, x = me_kv // 2, me_kv % 2
    tps = [(dy, dc) for dy in range(ny) for dc in range(2)]
    kvs = [(dz, dx) for dz in range(nz) for dx in range(2)]

    def tp_at(dy, dc):
        return ((y + dy + ny) % ny) * 2 + (core + dc + 2) % 2

    def kv_at(dz, dx):
        return ((z + dz + nz) % nz) * 2 + (x + dx + 2) % 2

    wcopies = []
    for d, (dy, dc) in enumerate(tps):
        src = tp_at(-dy, -dc)
        group = []
        for j, w in enumerate((wq_h, wk_h, wv_h, wo_h)):
            cp = pltpu.make_async_copy(
                w.at[pl.ds(pl.multiple_of(src * width, width), width), :],
                wqkv.at[d, :, pl.ds(j * cols, cols)],
                w_sem.at[d, j],
            )
            cp.start()
            group.append(cp)
        wcopies.append(group)
    mcopy = pltpu.make_async_copy(mem_h, mem, m_sem.at[0])
    mcopy.start()
    pcopies = []
    for d, (dy, dc) in enumerate(tps):
        src = tp_at(-dy, -dc)
        cp = pltpu.make_async_copy(
            wp_h.at[pl.ds(pl.multiple_of(src * cols, cols), cols), :], wp.at[d], p_sem.at[d]
        )
        cp.start()
        pcopies.append(cp)
    fcopies = []
    for i in range(2):
        at = pl.ds(pl.multiple_of(((core + i) % 2) * half, half), half)
        for j, (s, t) in enumerate(((wu_h.at[:, at], wu.at[i]), (wd_h.at[at, :], wd.at[i]))):
            cp = pltpu.make_async_copy(s, t, f_sem.at[i, j])
            cp.start()
            fcopies.append(cp)

    barrier = pltpu.get_barrier_semaphore()
    for dy, dc in tps[1:]:
        pl.semaphore_signal(
            barrier, inc=1, device_id={"tp": tp_at(dy, dc)}, device_id_type=pl.DeviceIdType.MESH
        )
    for dz, dx in kvs[1:]:
        pl.semaphore_signal(
            barrier, inc=1, device_id={"kv": kv_at(dz, dx)}, device_id_type=pl.DeviceIdType.MESH
        )
    pl.semaphore_wait(barrier, ntp + nkv - 2)

    sends = []

    def send(src, dst, s_sem, r_sem, device):
        cp = pltpu.make_async_remote_copy(
            src_ref=src,
            dst_ref=dst,
            send_sem=s_sem,
            recv_sem=r_sem,
            device_id=device,
            device_id_type=pl.DeviceIdType.MESH,
        )
        cp.start()
        sends.append(cp)
        return cp

    tok_in = [None]
    for d, (dy, dc) in enumerate(tps):
        if d:
            tok_in.append(
                send(tok, tokg.at[d], tp_send.at[d], tp_recv.at[d], {"tp": tp_at(dy, dc)})
            )
    acc = jnp.zeros((rows, 4 * cols), F32)
    in_acc = jnp.zeros((rows, wig.shape[1]), F32)
    fg_acc = jnp.zeros((rows, wig.shape[1]), F32)
    square = jnp.zeros((rows, 1), F32)
    for d, (dy, dc) in enumerate(tps):
        src = tp_at(-dy, -dc)
        at = pl.ds(pl.multiple_of(src * width, width), width)
        if d:
            tok_in[d].wait_recv()
        block = (tokg[d] if d else tok[...]).astype(F32)
        square += jnp.sum(block * block, axis=1, keepdims=True)
        gained = (block * ngain[:, at]).astype(BF16)
        for cp in wcopies[d]:
            cp.wait()
        acc += dot(gained, wqkv[d])
        in_acc += dot(gained, wig[at, :])
        fg_acc += dot(gained, wfg[at, :])
    scale = lax.rsqrt(square / features + EPS)
    acc = acc * scale
    lane = lax.broadcasted_iota(jnp.int32, in_acc.shape, 1)
    in_acc = in_acc * scale
    fg_acc = jax.nn.log_sigmoid(fg_acc * scale + fbias[...])

    mcopy.wait()
    pick = lax.broadcasted_iota(jnp.int32, (GROUP, dk), 0)
    for h in range(heads):
        mine = lane == me_tp * heads + h
        input_log = jnp.sum(jnp.where(mine, in_acc, 0.0), axis=1, keepdims=True)
        forget_log = jnp.sum(jnp.where(mine, fg_acc, 0.0), axis=1, keepdims=True)
        query, keys, values, gate = (
            acc[:, j * cols + h * dk : j * cols + (h + 1) * dk].astype(BF16) for j in range(4)
        )
        query_f, values_f, gate_f = query.astype(F32), values.astype(F32), gate.astype(F32)
        keys_f = keys.astype(F32) * dk**-0.5
        carried = forget_log + stab[:, h : h + 1]
        newest = jnp.maximum(carried, input_log)
        keep = jnp.exp(carried - newest)
        admit = jnp.exp(input_log - newest)
        norm_h = keep * nrm[:, h, :] + admit * keys_f
        nrm_new[:, h, :] = norm_h
        stab_new[:, h : h + 1] = newest
        keep_out[:, h : h + 1] = keep
        av_out[:, h, :] = admit * values_f
        key_out[:, h, :] = keys_f
        read = []
        for g in range(rows // GROUP):
            m = mem[g * GROUP : (g + 1) * GROUP, h].reshape(GROUP * dk, dk).astype(BF16)
            r = lax.dot_general(
                query[g * GROUP : (g + 1) * GROUP],
                m,
                (((1,), (1,)), ((), ())),
                preferred_element_type=F32,
            )
            total = jnp.zeros((GROUP, dk), F32)
            for i in range(GROUP):
                total = jnp.where(pick == i, r[:, i * dk : (i + 1) * dk], total)
            read.append(total)
        held = jnp.concatenate(read, axis=0)
        numer = keep * held + (
            admit * jnp.sum(keys_f * query_f, axis=1, keepdims=True)
        ) * values_f
        denom = jnp.sum(norm_h * query_f, axis=1, keepdims=True)
        cell = numer / jnp.maximum(jnp.abs(denom), 1.0)
        mixed = cell * mgain[:, h * dk : (h + 1) * dk] * jax.nn.sigmoid(gate_f)
        mixg[0, :, h * dk : (h + 1) * dk] = mixed.astype(BF16)

    mix_in = [None]
    for d, (dy, dc) in enumerate(tps):
        if d:
            mix_in.append(
                send(mixg.at[0], mixg.at[d], mx_send.at[d], mx_recv.at[d], {"tp": tp_at(dy, dc)})
            )
    second = tok[...].astype(F32)
    for d in range(ntp):
        if d:
            mix_in[d].wait_recv()
        pcopies[d].wait()
        second += dot(mixg[d], wp[d])
    secg[0, 0] = second.astype(BF16)

    sec_in = {}
    for dz, dx in kvs[1:]:
        sec_in[dz, dx] = send(
            secg.at[0, 0],
            secg.at[dz, dx],
            kv_send.at[dz, dx],
            kv_recv.at[dz, dx],
            {"kv": kv_at(dz, dx)},
        )
    for cp in fcopies:
        cp.wait()

    a_in, b_in, c_in, q_in, r_in = {}, {}, {}, {}, {}
    other_core = {"tp": tp_at(0, 1)}

    def stage1(c):
        for dx in range(2):
            if (c, dx) != (0, 0):
                sec_in[c, dx].wait_recv()
        block = secg[c].reshape(2 * rows, width).astype(F32)
        scaled = (block * fgain[...]).astype(BF16)
        xa_s[c] = dot(scaled, wu[1]).astype(BF16)
        a_in[c] = send(xa_s.at[c], xa_r.at[c], a_send.at[c], a_recv.at[c], other_core)
        squares = jnp.sum(block * block, axis=1, keepdims=True)
        wide = jnp.concatenate(
            [
                jnp.broadcast_to(squares, (2 * rows, LANES)),
                jnp.zeros((LANES - 2 * rows, LANES), F32),
            ],
            axis=0,
        )
        sq_s[c] = jnp.transpose(wide)[:8]
        q_in[c] = [
            send(
                sq_s.at[c],
                sq_r.at[c, d - 1],
                q_send.at[c, d - 1],
                q_recv.at[c, d - 1],
                {"tp": tp_at(*tps[d])},
            )
            for d in range(1, ntp)
        ]
        pown[c] = dot(scaled, wu[0])

    def stage2(c):
        a_in[c].wait_recv()
        both = pown[c] + xa_r[c].astype(F32)
        pown[c] = both
        yb_s[c] = both.astype(BF16)
        b_in[c] = [
            send(
                yb_s.at[c],
                yb_r.at[c, d - 1],
                b_send.at[c, d - 1],
                b_recv.at[c, d - 1],
                {"tp": tp_at(d, 0)},
            )
            for d in range(1, ny)
        ]

    def stage3(c):
        total = sq_s[c]
        for d in range(ntp - 1):
            q_in[c][d].wait_recv()
            total = total + sq_r[c, d]
        tall = jnp.transpose(jnp.broadcast_to(total[0:1], (LANES, LANES)))
        scale_two = lax.rsqrt(tall[: 2 * rows, 0:1] / features + EPS)
        summed = pown[c]
        for d in range(ny - 1):
            b_in[c][d].wait_recv()
            summed = summed + yb_r[c, d].astype(F32)
        hid[c] = jnp.square(jnp.maximum(summed * scale_two, 0.0)).astype(BF16)
        c_in[c] = send(hid.at[c], hid_r.at[c], c_send.at[c], c_recv.at[c], other_core)

    def stage4(c):
        part = dot(hid[c], wd[0])
        c_in[c].wait_recv()
        part = part + dot(hid_r[c], wd[1])
        for dx in range(2):
            piece = part[dx * rows : (dx + 1) * rows]
            if (c, dx) == (0, 0):
                down_own[...] = piece
                continue
            part_s[c, dx] = piece.astype(BF16)
            r_in[c, dx] = send(
                part_s.at[c, dx],
                part_r.at[c, dx],
                r_send.at[c, dx],
                r_recv.at[c, dx],
                {"kv": kv_at(-c, dx)},
            )

    for t in range(nz + LAG4):
        for lag, stage in ((0, stage1), (LAG2, stage2), (LAG3, stage3), (LAG4, stage4)):
            if 0 <= t - lag < nz:
                stage(t - lag)

    result = secg[0, 0].astype(F32) + down_own[...]
    for dz, dx in kvs[1:]:
        r_in[dz, dx].wait_recv()
        result += part_r[dz, dx].astype(F32)
    out[...] = result.astype(BF16)
    for cp in sends:
        cp.wait_send()


def per_device(
    nkv,
    ntp,
    tokens,
    memory,
    normalizer,
    stabilizer,
    norm_gain,
    query_weight,
    key_weight,
    value_weight,
    outgate_weight,
    input_gate_weight,
    forget_gate_weight,
    forget_bias,
    memory_gain,
    proj_weight,
    ffn_gain,
    up_weight,
    down_weight,
):
    rows, width = tokens.shape
    heads, dk = normalizer.shape[1:]
    cols = heads * dk
    half = up_weight.shape[1] // 2
    ny, nz = ntp // 2, nkv // 2
    shape = jax.ShapeDtypeStruct
    vmem = pl.BlockSpec(memory_space=pltpu.VMEM)
    hbm = pl.BlockSpec(memory_space=pl.ANY)
    dma = pltpu.SemaphoreType.DMA
    chunk = (nz, 2 * rows, half)
    blocks = (nz, 2, rows, width)
    out, nrm_new, stab_new, keep, av, keys = pl.pallas_call(
        functools.partial(layer_kernel, nkv, ntp),
        out_shape=(
            shape((rows, width), BF16),
            shape((rows, heads, dk), F32),
            shape((rows, heads), F32),
            shape((rows, heads), F32),
            shape((rows, heads, dk), F32),
            shape((rows, heads, dk), F32),
        ),
        in_specs=[
            vmem, hbm, vmem, vmem, vmem, hbm, hbm, hbm, hbm, vmem, vmem, vmem, vmem, hbm, vmem,
            hbm, hbm,
        ],
        out_specs=(vmem,) * 6,
        scratch_shapes=[
            pltpu.VMEM(memory.shape, F32),
            pltpu.VMEM((ntp, width, 4 * cols), BF16),
            pltpu.VMEM((ntp, cols, width), BF16),
            pltpu.VMEM((2, width, half), BF16),
            pltpu.VMEM((2, half, width), BF16),
            pltpu.VMEM((ntp, rows, width), BF16),
            pltpu.VMEM((ntp, rows, cols), BF16),
            pltpu.VMEM(blocks, BF16),
            pltpu.VMEM(chunk, F32),
            pltpu.VMEM(chunk, BF16),
            pltpu.VMEM(chunk, BF16),
            pltpu.VMEM(chunk, BF16),
            pltpu.VMEM((nz, ny - 1, 2 * rows, half), BF16),
            pltpu.VMEM(chunk, BF16),
            pltpu.VMEM(chunk, BF16),
            pltpu.VMEM((nz, 8, LANES), F32),
            pltpu.VMEM((nz, ntp - 1, 8, LANES), F32),
            pltpu.VMEM(blocks, BF16),
            pltpu.VMEM(blocks, BF16),
            pltpu.VMEM((rows, width), F32),
            dma((ntp, 4)),
            dma((ntp,)),
            dma((2, 2)),
            dma((1,)),
            dma((ntp,)),
            dma((ntp,)),
            dma((ntp,)),
            dma((ntp,)),
            dma((nz, 2)),
            dma((nz, 2)),
            dma((nz,)),
            dma((nz,)),
            dma((nz, ny - 1)),
            dma((nz, ny - 1)),
            dma((nz,)),
            dma((nz,)),
            dma((nz, ntp - 1)),
            dma((nz, ntp - 1)),
            dma((nz, 2)),
            dma((nz, 2)),
        ],
        compiler_params=pltpu.CompilerParams(collective_id=0, has_side_effects=True),
        name="layer",
    )(
        tokens,
        memory,
        normalizer,
        stabilizer,
        norm_gain[None, :],
        query_weight,
        key_weight,
        value_weight,
        outgate_weight,
        input_gate_weight,
        forget_gate_weight,
        forget_bias[None, :],
        memory_gain[None, :],
        proj_weight,
        ffn_gain[None, :],
        up_weight,
        down_weight,
    )
    memory_new = keep[..., None, None] * memory + av[..., :, None] * keys[..., None, :]
    return (out, memory_new, nrm_new, stab_new)


def solution(mesh):
    placed = (
        P("kv", "tp"),
        P("kv", "tp", None, None),
        P("kv", "tp", None),
        P("kv", "tp"),
        P(),
        P(None, "tp"),
        P(None, "tp"),
        P(None, "tp"),
        P(None, "tp"),
        P(),
        P(),
        P(),
        P("tp"),
        P(None, "tp"),
        P("tp"),
        P("tp", "kv"),
        P("kv", "tp"),
    )
    return jax.shard_map(
        functools.partial(per_device, mesh.shape["kv"], mesh.shape["tp"]),
        mesh=mesh,
        in_specs=placed,
        out_specs=(P("kv", "tp"), P("kv", "tp", None, None), P("kv", "tp", None), P("kv", "tp")),
        check_vma=False,
    )
```

```python
import functools

import jax
import jax.numpy as jnp
from jax import lax
from jax.experimental import pallas as pl
from jax.experimental.pallas import tpu as pltpu
from jax.sharding import PartitionSpec as P

EPS = 1e-06
LANES = 128
GROUP = 16
LAG2, LAG3, LAG4 = 1, 2, 3
F32, BF16 = jnp.float32, jnp.bfloat16


def dot(a, b):
    return jnp.dot(a, b, preferred_element_type=F32)


def dot_nt(a, b):
    return lax.dot_general(a, b, (((1,), (1,)), ((), ())), preferred_element_type=F32)


def layer_kernel(
    nkv,
    ntp,
    tok_h,
    mem_h,
    nrm_h,
    stab_h,
    ngain_h,
    wq_h,
    wk_h,
    wv_h,
    wo_h,
    wig_h,
    wfg_h,
    fbias_h,
    mgain_h,
    wp_h,
    fgain_h,
    wu_h,
    wd_h,
    out,
    nrm_new,
    stab_new,
    mem,
    nrm,
    stab,
    ngain,
    wig,
    wfg,
    fbias,
    mgain,
    fgain,
    mem_b,
    rowed,
    wqkv,
    wp,
    wu,
    wd,
    tokg,
    mixg,
    secg,
    pown,
    xa_s,
    xa_r,
    yb_s,
    yb_r,
    hid,
    hid_r,
    sq_s,
    sq_r,
    part_s,
    part_r,
    down_own,
    s_sem,
    w_sem,
    p_sem,
    f_sem,
    m_sem,
    tp_send,
    tp_recv,
    mx_send,
    mx_recv,
    kv_send,
    kv_recv,
    a_send,
    a_recv,
    b_send,
    b_recv,
    c_send,
    c_recv,
    q_send,
    q_recv,
    r_send,
    r_recv,
):
    rows, width = tok_h.shape
    tok = tokg.at[0]
    heads, dk = nrm.shape[1], nrm.shape[2]
    cols = heads * dk
    features = width * ntp
    half = wu.shape[2]
    ny, nz = ntp // 2, nkv // 2
    me_tp, me_kv = lax.axis_index("tp"), lax.axis_index("kv")
    y, core = me_tp // 2, me_tp % 2
    z, x = me_kv // 2, me_kv % 2
    tps = [(dy, dc) for dy in range(ny) for dc in range(2)]
    kvs = [(dz, dx) for dz in range(nz) for dx in range(2)]

    def tp_at(dy, dc):
        return ((y + dy + ny) % ny) * 2 + (core + dc + 2) % 2

    def kv_at(dz, dx):
        return ((z + dz + nz) % nz) * 2 + (x + dx + 2) % 2

    small = [
        pltpu.make_async_copy(s, t, s_sem.at[i])
        for i, (s, t) in enumerate(
            (
                (tok_h, tok),
                (ngain_h, ngain),
                (wig_h, wig),
                (wfg_h, wfg),
                (fbias_h, fbias),
                (stab_h, stab),
                (nrm_h, nrm),
                (mgain_h, mgain),
                (fgain_h, fgain),
            )
        )
    ]
    for cp in small:
        cp.start()
    wcopies = []
    for d, (dy, dc) in enumerate(tps):
        src = tp_at(-dy, -dc)
        group = []
        for j, w in enumerate((wq_h, wk_h, wv_h, wo_h)):
            cp = pltpu.make_async_copy(
                w.at[pl.ds(pl.multiple_of(src * width, width), width), :],
                wqkv.at[d, :, pl.ds(j * cols, cols)],
                w_sem.at[d, j],
            )
            cp.start()
            group.append(cp)
        wcopies.append(group)
    mcopy = pltpu.make_async_copy(mem_h, mem, m_sem.at[0])
    mcopy.start()
    pcopies = []
    for d, (dy, dc) in enumerate(tps):
        src = tp_at(-dy, -dc)
        cp = pltpu.make_async_copy(
            wp_h.at[pl.ds(pl.multiple_of(src * cols, cols), cols), :], wp.at[d], p_sem.at[d]
        )
        cp.start()
        pcopies.append(cp)
    fcopies = []
    for i in range(2):
        at = pl.ds(pl.multiple_of(((core + i) % 2) * half, half), half)
        for j, (s, t) in enumerate(((wu_h.at[:, at], wu.at[i]), (wd_h.at[at, :], wd.at[i]))):
            cp = pltpu.make_async_copy(s, t, f_sem.at[i, j])
            cp.start()
            fcopies.append(cp)

    barrier = pltpu.get_barrier_semaphore()
    for dy, dc in tps[1:]:
        pl.semaphore_signal(
            barrier, inc=1, device_id={"tp": tp_at(dy, dc)}, device_id_type=pl.DeviceIdType.MESH
        )
    for dz, dx in kvs[1:]:
        pl.semaphore_signal(
            barrier, inc=1, device_id={"kv": kv_at(dz, dx)}, device_id_type=pl.DeviceIdType.MESH
        )
    pl.semaphore_wait(barrier, ntp + nkv - 2)

    sends = []

    def send(src, dst, s_sem, r_sem, device):
        cp = pltpu.make_async_remote_copy(
            src_ref=src,
            dst_ref=dst,
            send_sem=s_sem,
            recv_sem=r_sem,
            device_id=device,
            device_id_type=pl.DeviceIdType.MESH,
        )
        cp.start()
        sends.append(cp)
        return cp

    small[0].wait()
    tok_in = [None]
    for d, (dy, dc) in enumerate(tps):
        if d:
            tok_in.append(
                send(tok, tokg.at[d], tp_send.at[d], tp_recv.at[d], {"tp": tp_at(dy, dc)})
            )
    for cp in small[1:]:
        cp.wait()
    acc = jnp.zeros((rows, 4 * cols), F32)
    in_acc = jnp.zeros((rows, wig.shape[0]), F32)
    fg_acc = jnp.zeros((rows, wig.shape[0]), F32)
    square = jnp.zeros((rows, 1), F32)
    for d, (dy, dc) in enumerate(tps):
        src = tp_at(-dy, -dc)
        at = pl.ds(pl.multiple_of(src * width, width), width)
        if d:
            tok_in[d].wait_recv()
        block = tokg[d].astype(F32)
        square += jnp.sum(block * block, axis=1, keepdims=True)
        gained = (block * ngain[:, at]).astype(BF16)
        for cp in wcopies[d]:
            cp.wait()
        acc += dot(gained, wqkv[d])
        in_acc += dot_nt(gained, wig[:, at])
        fg_acc += dot_nt(gained, wfg[:, at])
        if d == 0:
            mcopy.wait()
            for h in range(heads):
                for b in range(rows):
                    mem_b[h, b] = mem[b, h].astype(BF16)
    scale = lax.rsqrt(square / features + EPS)
    acc = acc * scale
    lane = lax.broadcasted_iota(jnp.int32, in_acc.shape, 1)
    in_acc = in_acc * scale
    fg_acc = jax.nn.log_sigmoid(fg_acc * scale + fbias[...])

    diagonal = lax.broadcasted_iota(jnp.int32, (rows, rows), 0) == lax.broadcasted_iota(
        jnp.int32, (rows, rows), 1
    )
    admitted = []
    pick = lax.broadcasted_iota(jnp.int32, (GROUP, dk), 0)
    for h in range(heads):
        mine = lane == me_tp * heads + h
        input_log = jnp.sum(jnp.where(mine, in_acc, 0.0), axis=1, keepdims=True)
        forget_log = jnp.sum(jnp.where(mine, fg_acc, 0.0), axis=1, keepdims=True)
        query, keys, values, gate = (
            acc[:, j * cols + h * dk : j * cols + (h + 1) * dk].astype(BF16) for j in range(4)
        )
        query_f, values_f, gate_f = query.astype(F32), values.astype(F32), gate.astype(F32)
        keys_f = keys.astype(F32) * dk**-0.5
        before = jnp.sum(
            jnp.where(diagonal, jnp.broadcast_to(stab[h : h + 1, :], (rows, rows)), 0.0),
            axis=1,
            keepdims=True,
        )
        carried = forget_log + before
        newest = jnp.maximum(carried, input_log)
        keep = jnp.exp(carried - newest)
        admit = jnp.exp(input_log - newest)
        norm_h = keep * nrm[:, h, :] + admit * keys_f
        nrm_new[:, h, :] = norm_h
        stab_new[h : h + 1, :] = jnp.sum(
            jnp.where(diagonal, jnp.broadcast_to(newest, (rows, rows)), 0.0), axis=0, keepdims=True
        )
        rowed[h, 0] = jnp.broadcast_to(keep, (rows, dk))
        rowed[h, 1] = keys_f
        admitted.append(admit * values_f)
        read = []
        for g in range(rows // GROUP):
            m = mem_b[h, g * GROUP : (g + 1) * GROUP].reshape(GROUP * dk, dk)
            r = dot_nt(query[g * GROUP : (g + 1) * GROUP], m)
            total = jnp.zeros((GROUP, dk), F32)
            for i in range(GROUP):
                total = jnp.where(pick == i, r[:, i * dk : (i + 1) * dk], total)
            read.append(total)
        held = jnp.concatenate(read, axis=0)
        numer = keep * held + (
            admit * jnp.sum(keys_f * query_f, axis=1, keepdims=True)
        ) * values_f
        denom = jnp.sum(norm_h * query_f, axis=1, keepdims=True)
        cell = numer / jnp.maximum(jnp.abs(denom), 1.0)
        mixed = cell * mgain[:, h * dk : (h + 1) * dk] * jax.nn.sigmoid(gate_f)
        mixg[0, :, h * dk : (h + 1) * dk] = mixed.astype(BF16)

    mix_in = [None]
    for d, (dy, dc) in enumerate(tps):
        if d:
            mix_in.append(
                send(mixg.at[0], mixg.at[d], mx_send.at[d], mx_recv.at[d], {"tp": tp_at(dy, dc)})
            )
    for h in range(heads):
        tall = jnp.transpose(
            jnp.concatenate([admitted[h], jnp.zeros((dk - rows, dk), F32)], axis=0)
        )
        for b in range(rows):
            mem[b, h] = rowed[h, 0, b : b + 1, :] * mem[b, h] + (
                tall[:, b : b + 1] * rowed[h, 1, b : b + 1, :]
            )

    second = tok[...].astype(F32)
    for d in range(ntp):
        if d:
            mix_in[d].wait_recv()
        pcopies[d].wait()
        second += dot(mixg[d], wp[d])
    secg[0, 0] = second.astype(BF16)

    sec_in = {}
    for dz, dx in kvs[1:]:
        sec_in[dz, dx] = send(
            secg.at[0, 0],
            secg.at[dz, dx],
            kv_send.at[dz, dx],
            kv_recv.at[dz, dx],
            {"kv": kv_at(dz, dx)},
        )
    for cp in fcopies:
        cp.wait()

    a_in, b_in, c_in, q_in, r_in = {}, {}, {}, {}, {}
    other_core = {"tp": tp_at(0, 1)}

    def stage1(c):
        for dx in range(2):
            if (c, dx) != (0, 0):
                sec_in[c, dx].wait_recv()
        block = secg[c].reshape(2 * rows, width).astype(F32)
        scaled = (block * fgain[...]).astype(BF16)
        xa_s[c] = dot(scaled, wu[1]).astype(BF16)
        a_in[c] = send(xa_s.at[c], xa_r.at[c], a_send.at[c], a_recv.at[c], other_core)
        squares = jnp.sum(block * block, axis=1, keepdims=True)
        wide = jnp.concatenate(
            [
                jnp.broadcast_to(squares, (2 * rows, LANES)),
                jnp.zeros((LANES - 2 * rows, LANES), F32),
            ],
            axis=0,
        )
        sq_s[c] = jnp.transpose(wide)[:8]
        q_in[c] = [
            send(
                sq_s.at[c],
                sq_r.at[c, d - 1],
                q_send.at[c, d - 1],
                q_recv.at[c, d - 1],
                {"tp": tp_at(*tps[d])},
            )
            for d in range(1, ntp)
        ]
        pown[c] = dot(scaled, wu[0])

    def stage2(c):
        a_in[c].wait_recv()
        both = pown[c] + xa_r[c].astype(F32)
        pown[c] = both
        yb_s[c] = both.astype(BF16)
        b_in[c] = [
            send(
                yb_s.at[c],
                yb_r.at[c, d - 1],
                b_send.at[c, d - 1],
                b_recv.at[c, d - 1],
                {"tp": tp_at(d, 0)},
            )
            for d in range(1, ny)
        ]

    def stage3(c):
        total = sq_s[c]
        for d in range(ntp - 1):
            q_in[c][d].wait_recv()
            total = total + sq_r[c, d]
        tall = jnp.transpose(jnp.broadcast_to(total[0:1], (LANES, LANES)))
        scale_two = lax.rsqrt(tall[: 2 * rows, 0:1] / features + EPS)
        summed = pown[c]
        for d in range(ny - 1):
            b_in[c][d].wait_recv()
            summed = summed + yb_r[c, d].astype(F32)
        hid[c] = jnp.square(jnp.maximum(summed * scale_two, 0.0)).astype(BF16)
        c_in[c] = send(hid.at[c], hid_r.at[c], c_send.at[c], c_recv.at[c], other_core)

    def stage4(c):
        part = dot(hid[c], wd[0])
        c_in[c].wait_recv()
        part = part + dot(hid_r[c], wd[1])
        for dx in range(2):
            piece = part[dx * rows : (dx + 1) * rows]
            if (c, dx) == (0, 0):
                down_own[...] = piece
                continue
            part_s[c, dx] = piece.astype(BF16)
            r_in[c, dx] = send(
                part_s.at[c, dx],
                part_r.at[c, dx],
                r_send.at[c, dx],
                r_recv.at[c, dx],
                {"kv": kv_at(-c, dx)},
            )

    for t in range(nz + LAG4):
        for lag, stage in ((0, stage1), (LAG2, stage2), (LAG3, stage3), (LAG4, stage4)):
            if 0 <= t - lag < nz:
                stage(t - lag)

    result = secg[0, 0].astype(F32) + down_own[...]
    for dz, dx in kvs[1:]:
        r_in[dz, dx].wait_recv()
        result += part_r[dz, dx].astype(F32)
    out[...] = result.astype(BF16)
    for cp in sends:
        cp.wait_send()


def put_kernel(*refs):
    sem = refs[-1]
    n = (len(refs) - 1) // 2
    copies = [pltpu.make_async_copy(refs[i], refs[n + i], sem.at[i]) for i in range(n)]
    for cp in reversed(copies):
        cp.start()
    for cp in copies:
        cp.wait()


def per_device(
    nkv,
    ntp,
    tokens,
    memory,
    normalizer,
    stabilizer,
    norm_gain,
    query_weight,
    key_weight,
    value_weight,
    outgate_weight,
    input_gate_weight,
    forget_gate_weight,
    forget_bias,
    memory_gain,
    proj_weight,
    ffn_gain,
    up_weight,
    down_weight,
):
    rows, width = tokens.shape
    heads, dk = normalizer.shape[1:]
    cols = heads * dk
    half = up_weight.shape[1] // 2
    ny, nz = ntp // 2, nkv // 2
    shape = jax.ShapeDtypeStruct
    vmem = pl.BlockSpec(memory_space=pltpu.VMEM)
    hbm = pl.BlockSpec(memory_space=pl.ANY)
    dma = pltpu.SemaphoreType.DMA
    far = functools.partial(pltpu.with_memory_space_constraint, memory_space=pltpu.HBM)
    chunk = (nz, 2 * rows, half)
    blocks = (nz, 2, rows, width)
    whole = (
        ((rows, width), BF16),
        ((rows, heads, dk), F32),
        ((heads, rows), F32),
        (memory.shape, F32),
    )
    made = pl.pallas_call(
        functools.partial(layer_kernel, nkv, ntp),
        out_shape=tuple(pltpu.VMEM(*w) for w in whole),
        in_specs=[hbm] * 17,
        out_specs=(vmem,) * 4,
        scratch_shapes=[
            pltpu.VMEM(normalizer.shape, F32),
            pltpu.VMEM((heads, rows), F32),
            pltpu.VMEM((1, width * ntp), F32),
            pltpu.VMEM(input_gate_weight.shape[::-1], BF16),
            pltpu.VMEM(input_gate_weight.shape[::-1], BF16),
            pltpu.VMEM((1, heads * ntp), F32),
            pltpu.VMEM((1, cols), F32),
            pltpu.VMEM((1, width), F32),
            pltpu.VMEM((heads, rows, dk, dk), BF16),
            pltpu.VMEM((heads, 2, rows, dk), F32),
            pltpu.VMEM((ntp, width, 4 * cols), BF16),
            pltpu.VMEM((ntp, cols, width), BF16),
            pltpu.VMEM((2, width, half), BF16),
            pltpu.VMEM((2, half, width), BF16),
            pltpu.VMEM((ntp, rows, width), BF16),
            pltpu.VMEM((ntp, rows, cols), BF16),
            pltpu.VMEM(blocks, BF16),
            pltpu.VMEM(chunk, F32),
            pltpu.VMEM(chunk, BF16),
            pltpu.VMEM(chunk, BF16),
            pltpu.VMEM(chunk, BF16),
            pltpu.VMEM((nz, ny - 1, 2 * rows, half), BF16),
            pltpu.VMEM(chunk, BF16),
            pltpu.VMEM(chunk, BF16),
            pltpu.VMEM((nz, 8, LANES), F32),
            pltpu.VMEM((nz, ntp - 1, 8, LANES), F32),
            pltpu.VMEM(blocks, BF16),
            pltpu.VMEM(blocks, BF16),
            pltpu.VMEM((rows, width), F32),
            dma((9,)),
            dma((ntp, 4)),
            dma((ntp,)),
            dma((2, 2)),
            dma((1,)),
            dma((ntp,)),
            dma((ntp,)),
            dma((ntp,)),
            dma((ntp,)),
            dma((nz, 2)),
            dma((nz, 2)),
            dma((nz,)),
            dma((nz,)),
            dma((nz, ny - 1)),
            dma((nz, ny - 1)),
            dma((nz,)),
            dma((nz,)),
            dma((nz, ntp - 1)),
            dma((nz, ntp - 1)),
            dma((nz, 2)),
            dma((nz, 2)),
        ],
        compiler_params=pltpu.CompilerParams(
            collective_id=0, has_side_effects=True, vmem_limit_bytes=40 * 2**20
        ),
        name="layer",
    )(
        *map(
            far,
            (
                tokens,
                memory,
                normalizer,
                stabilizer.T,
                norm_gain[None, :],
                query_weight,
                key_weight,
                value_weight,
                outgate_weight,
                input_gate_weight.T,
                forget_gate_weight.T,
                forget_bias[None, :],
                memory_gain[None, :],
                proj_weight,
                ffn_gain[None, :],
                up_weight,
                down_weight,
            ),
        )
    )
    out, nrm_new, stab_new, memory_new = pl.pallas_call(
        put_kernel,
        out_shape=tuple(shape(*w) for w in whole),
        in_specs=[vmem] * 4,
        out_specs=(hbm,) * 4,
        scratch_shapes=[dma((4,))],
        compiler_params=pltpu.CompilerParams(vmem_limit_bytes=2**20),
        name="put",
    )(*made)
    return (out, memory_new, nrm_new, stab_new.T)


def solution(mesh):
    placed = (
        P("kv", "tp"),
        P("kv", "tp", None, None),
        P("kv", "tp", None),
        P("kv", "tp"),
        P(),
        P(None, "tp"),
        P(None, "tp"),
        P(None, "tp"),
        P(None, "tp"),
        P(),
        P(),
        P(),
        P("tp"),
        P(None, "tp"),
        P("tp"),
        P("tp", "kv"),
        P("kv", "tp"),
    )
    return jax.shard_map(
        functools.partial(per_device, mesh.shape["kv"], mesh.shape["tp"]),
        mesh=mesh,
        in_specs=placed,
        out_specs=(P("kv", "tp"), P("kv", "tp", None, None), P("kv", "tp", None), P("kv", "tp")),
        check_vma=False,
    )
```
